32 devices in a mesh: fs: 8 (over z, y), tp: 4 (over x, core).
Axes of the slice: x: 2, y: 2, z: 4, core: 2. Of those that a mesh axis runs over, the one named last changes fastest.
Arguments:
- saved_inputs: bfloat16 [16384, 4096], P('fs'), may hold values from -6 to 6
- value_cot: bfloat16 [16384, 1024], P('fs', 'tp'), may hold values from -6 to 6
- gate_cot: bfloat16 [16384, 1024], P('fs', 'tp'), may hold values from -6 to 6
- point_inputs: bfloat16 [16384, 1024], P('fs'), may hold values from -6 to 6
- point_cot: bfloat16 [16384, 1024], P('fs', 'tp'), may hold values from -6 to 6
- master_value: float32 [4096, 1024], P('fs', 'tp'), may hold values from -6 to 6
- master_gate: float32 [4096, 1024], P('fs', 'tp'), may hold values from -6 to 6
- master_point: float32 [1024, 1024], P('fs', 'tp'), may hold values from -6 to 6
- factor_value: bfloat16 [4096, 256], P('fs'), may hold values from -160 to 160
- factor_gate: bfloat16 [4096, 256], P('fs'), may hold values from -160 to 160
- factor_point: bfloat16 [1024, 256], P('fs'), may hold values from -160 to 160
- first_value: float32 [256, 1024], P('fs', 'tp'), may hold values from -6 to 6
- first_gate: float32 [256, 1024], P('fs', 'tp'), may hold values from -6 to 6
- first_point: float32 [256, 1024], P('fs', 'tp'), may hold values from -6 to 6
- second_value: float32 [256, 1024], P('fs', 'tp'), may hold values from 0.2 to 2
- second_gate: float32 [256, 1024], P('fs', 'tp'), may hold values from 0.2 to 2
- second_point: float32 [256, 1024], P('fs', 'tp'), may hold values from 0.2 to 2
Outputs:
- new_value: float32 [4096, 1024], P('fs', 'tp')
- new_gate: float32 [4096, 1024], P('fs', 'tp')
- new_point: float32 [1024, 1024], P('fs', 'tp')
- copy_value: bfloat16 [4096, 1024], P(None, 'tp')
- copy_gate: bfloat16 [4096, 1024], P(None, 'tp')
- copy_point: bfloat16 [1024, 1024], P(None, 'tp')
- next_first_value: float32 [256, 1024], P('fs', 'tp')
- next_first_gate: float32 [256, 1024], P('fs', 'tp')
- next_first_point: float32 [256, 1024], P('fs', 'tp')
- next_second_value: float32 [256, 1024], P('fs', 'tp')
- next_second_gate: float32 [256, 1024], P('fs', 'tp')
- next_second_point: float32 [256, 1024], P('fs', 'tp')
The draws below stay inside these ranges and needn't reach their ends.
All inputs are finite; a program needn't handle non-finite values.
Results may differ from the reference program's by a relative error of at most 0.0055.
Values may be sent and summed in bfloat16 or wider, within the bound.
A program may use at most 128 MiB of HBM per device.

```python
import math
import jax
import jax.numpy as jnp
from jax import lax

D = 4096
C = 1024
RANK = 256
TOKENS = 16384


def factor_rows(key, rows):
    k_base, k_scale = jax.random.split(jax.random.fold_in(key, 7))
    place = jnp.arange(rows, dtype=jnp.float32) / max(rows - 1, 1)
    spread = jnp.exp(jax.random.uniform(k_scale, (rows, 1), jnp.float32) * jnp.log(10.0))
    base = jnp.clip(jax.random.normal(k_base, (rows, RANK), jnp.float32), -3.0, 3.0)
    ramp = jnp.exp(place * jnp.log(3.0))
    return (base * ramp[:, None] * spread).astype(jnp.bfloat16)


def draw_factor_value(key, part):
    return factor_rows(jax.random.fold_in(key, 1), D)


def draw_factor_gate(key, part):
    return factor_rows(jax.random.fold_in(key, 2), D)


def draw_factor_point(key, part):
    return factor_rows(jax.random.fold_in(key, 3), C)


def levels(own_key, dims, cuts, low, top_value):
    def one(dim, blocks):
        draws = jax.random.uniform(jax.random.fold_in(jax.random.fold_in(own_key, 6), dim), (blocks,), jnp.float32, low / len(cuts), top_value / len(cuts))
        return jnp.repeat(jnp.exp(draws), dims[dim] // blocks).reshape((-1,) + (1,) * (len(dims) - dim - 1))

    level = one(*cuts[0])
    for cut in cuts[1:]:
        level = level * one(*cut)
    return level


def noise(own_key, extent, scale, reach, cuts=(), kind=jnp.bfloat16):
    drawn = jax.random.normal(own_key, extent, jnp.float32) * scale
    if len(cuts) > 0:
        drawn = levels(own_key, extent, cuts, -0.22, 0.18) * drawn
    return jnp.clip(drawn, min=-reach, max=reach).astype(kind)


def setup_inputs(seed: int = 0) -> dict:
    keys = jax.random.split(jax.random.key(seed), 18)
    saved_inputs = noise(keys[0], (TOKENS, D), 1.0, 6.0, ((0, 8),))
    value_cot = noise(keys[1], (TOKENS, C), 1.0, 6.0, ((0, 8), (1, 4)))
    gate_cot = noise(keys[2], (TOKENS, C), 1.0, 6.0, ((0, 8), (1, 4)))
    point_inputs = noise(keys[3], (TOKENS, C), 1.0, 6.0, ((0, 8),))
    point_cot = noise(keys[4], (TOKENS, C), 1.0, 6.0, ((0, 8), (1, 4)))
    master_value = noise(keys[5], (D, C), 1.0, 6.0, ((0, 8), (1, 4)), jnp.float32)
    master_gate = noise(keys[6], (D, C), 1.0, 6.0, ((0, 8), (1, 4)), jnp.float32)
    master_point = noise(keys[7], (C, C), 1.0, 6.0, ((0, 8), (1, 4)), jnp.float32)
    factor_value = draw_factor_value(jax.random.fold_in(keys[17], 71), 0)
    factor_gate = draw_factor_gate(jax.random.fold_in(keys[17], 71), 0)
    factor_point = draw_factor_point(jax.random.fold_in(keys[17], 71), 0)
    first_value = noise(keys[11], (RANK, C), 1.0, 6.0, ((0, 8), (1, 4)), jnp.float32)
    first_gate = noise(keys[12], (RANK, C), 1.0, 6.0, ((0, 8), (1, 4)), jnp.float32)
    first_point = noise(keys[13], (RANK, C), 1.0, 6.0, ((0, 8), (1, 4)), jnp.float32)
    second_value = jnp.clip(jnp.exp(math.log(2.0) - 2.3025851 * jax.random.uniform(keys[14], (RANK, C), jnp.float32) ** levels(keys[14], (RANK, C), ((0, 8), (1, 4)), -0.2, 0.2)), 0.2, 2.0)
    second_gate = jnp.clip(jnp.exp(math.log(2.0) - 2.3025851 * jax.random.uniform(keys[15], (RANK, C), jnp.float32) ** levels(keys[15], (RANK, C), ((0, 8), (1, 4)), -0.2, 0.2)), 0.2, 2.0)
    second_point = jnp.clip(jnp.exp(math.log(2.0) - 2.3025851 * jax.random.uniform(keys[16], (RANK, C), jnp.float32) ** levels(keys[16], (RANK, C), ((0, 8), (1, 4)), -0.2, 0.2)), 0.2, 2.0)
    return {"saved_inputs": saved_inputs, "value_cot": value_cot, "gate_cot": gate_cot, "point_inputs": point_inputs, "point_cot": point_cot, "master_value": master_value, "master_gate": master_gate, "master_point": master_point, "factor_value": factor_value, "factor_gate": factor_gate, "factor_point": factor_point, "first_value": first_value, "first_gate": first_gate, "first_point": first_point, "second_value": second_value, "second_gate": second_gate, "second_point": second_point}


def low_part(inputs, cot, factor):
    projected = jnp.dot(inputs, factor, preferred_element_type=jnp.float32)
    summed = lax.dot_general(projected, cot.astype(jnp.float32), (((0,), (0,)), ((), ())), precision=lax.Precision.HIGHEST, preferred_element_type=jnp.float32)
    return summed / TOKENS

def update(master, factor, low, first_old, second_old):
    first = 0.8 * first_old + 0.2 * low
    second = 0.9 * second_old + 0.1 * low * low
    direction = first / (jnp.sqrt(second) + 1e-08)
    full = jnp.dot(factor.astype(jnp.float32), direction, precision=lax.Precision.HIGHEST)
    scale = lax.rsqrt(jnp.mean(full * full) + 1e-06)
    new = master - 0.1 * scale * full
    return (new, new.astype(jnp.bfloat16), first, second)

def reference(saved_inputs, value_cot, gate_cot, point_inputs, point_cot, master_value, master_gate, master_point, factor_value, factor_gate, factor_point, first_value, first_gate, first_point, second_value, second_gate, second_point):
    low_value = low_part(saved_inputs, value_cot, factor_value)
    low_gate = low_part(saved_inputs, gate_cot, factor_gate)
    low_point = low_part(point_inputs, point_cot, factor_point)
    nv, cv, fv, sv = update(master_value, factor_value, low_value, first_value, second_value)
    ng, cg, fg, sg = update(master_gate, factor_gate, low_gate, first_gate, second_gate)
    npt, cpt, fpt, spt = update(master_point, factor_point, low_point, first_point, second_point)
    return (nv, ng, npt, cv, cg, cpt, fv, fg, fpt, sv, sg, spt)
```

```python
import functools

import jax
import jax.numpy as jnp
from jax import lax
from jax.experimental import pallas as pl
from jax.experimental.pallas import tpu as pltpu
from jax.sharding import PartitionSpec as P

MESH = pl.DeviceIdType.MESH
F32 = jnp.float32
BF16 = jnp.bfloat16


def tile_of(total, most):
    size = min(total, most)
    while total % size:
        size -= 8
    return size


def ring_position(index, n):
    half, odd = index // 2, index % 2
    return half + odd * (n - 1 - 2 * half)


def ring_index(position, n):
    back = position // (n // 2)
    return 2 * (position + back * (n - 1 - 2 * position)) + back


class Plan:
    def __init__(self, send, recv):
        self.send, self.recv, self.names, self.sent = send, recv, {}, []

    def copy(self, name, src, dst, device):
        slot = self.names.setdefault(name, len(self.names))
        return pltpu.make_async_remote_copy(
            src_ref=src, dst_ref=dst, send_sem=self.send.at[slot], recv_sem=self.recv.at[slot],
            device_id=device, device_id_type=MESH,
        )

    def start(self, name, src, dst, device):
        copy = self.copy(name, src, dst, device)
        copy.start()
        self.sent.append(copy)

    def arrived(self, name, dst, device):
        self.copy(name, dst, dst, device).wait_recv()

    def drain(self):
        for copy in self.sent:
            copy.wait_send()


def kernel(
    n, m, splits,
    x, xp, yv, yg, yp, mv, mg, mp, fv, fg, fp,
    f0, f1, f2, s0, s1, s2,
    out_pv, out_pg, out_pp, out_mv, out_mg, out_mp, out_low, out_dir, out_ss,
    xbuf, xpbuf, ybuf, vg, pp, mvg, mpp, m32, mp32, acc, lows, low_send, low_recv, dir_all, ss_own, ss_all,
    send, recv, local,
):
    fs, tp = lax.axis_index("fs"), lax.axis_index("tp")
    here = ring_position(fs, n)
    right = {"fs": ring_index((here + 1) % n, n)}
    left = {"fs": ring_index((here + n - 1) % n, n)}
    pairs = m // 2
    q, c = tp // 2, tp % 2
    partner = {"tp": 2 * q + 1 - c}
    rows, rows_p = fv.shape[0], fp.shape[0]
    tokens = x.shape[0]
    rank = vg.shape[2]
    part = rank // n
    half = n // 2
    net = Plan(send, recv)
    slots = iter(range(local.shape[0]))

    def fetch(src, dst):
        copy = pltpu.make_async_copy(src, dst, local.at[next(slots)])
        copy.start()
        return copy

    def block(event):
        if event == 0:
            return fs
        step = (event + 1) // 2
        return ring_index((here + (n - step if event % 2 else step)) % n, n)

    blocks = [block(e) for e in range(n)]

    def span(start, size, align):
        return pl.ds(pl.multiple_of(start, align), size)

    own = span(fs * rows, rows, rows)
    own_p = span(fs * rows_p, rows_p, rows_p)
    factor_in = [
        fetch(fp, pp.at[own_p]), fetch(fv, vg.at[0, own]), fetch(fg, vg.at[1, own]),
    ]
    master_in = [fetch(mv, m32.at[0]), fetch(mg, m32.at[1]), fetch(mp, mp32)]
    x_in = []
    for e in range(n):
        x_in.append(fetch(x.at[:, span(blocks[e] * rows, rows, rows)], xbuf.at[e]))
        if e == 0:
            xp_in = fetch(xp, xpbuf)
    y_in = [fetch(yv, ybuf.at[0]), fetch(yg, ybuf.at[1]), fetch(yp, ybuf.at[2])]

    barrier = pltpu.get_barrier_semaphore()
    for d in range(1, n):
        pl.semaphore_signal(barrier, inc=1, device_id={"fs": (fs + d) % n}, device_id_type=MESH)
    for d in range(1, m):
        pl.semaphore_signal(barrier, inc=1, device_id={"tp": (tp + d) % m}, device_id_type=MESH)
    for copy in factor_in:
        copy.wait()
    pl.semaphore_wait(barrier, n - 1 + m - 1)

    def piece(ref, owner, lo, size, align):
        if len(ref.shape) == 3:
            return ref.at[:, span(owner, size, align)] if lo is None else ref.at[:, span(owner + lo, size, align)]
        return ref.at[span(owner, size, align)] if lo is None else ref.at[span(owner + lo, size, align)]

    def stream(name, ref, size, split):
        sent = size // split
        offset = 0 if split == 1 else tp * sent
        return (name, ref, size, offset, sent)

    factors = [stream("p", pp, rows_p, splits[1]), stream("vg", vg, rows, splits[0])]
    masters = [stream("mvg", mvg, rows, 1), stream("mp", mpp, rows_p, 1)]

    def ring_piece(item, event, way):
        name, ref, size, offset, sent = item
        last = event == n - 1
        if last:
            cut = sent // 2
            return piece(ref, blocks[event] * size + offset + way * cut, None, cut, cut)
        return piece(ref, blocks[event] * size + offset, None, sent, sent)

    def ring_send(item, step):
        for way, device in ((0, right), (1, left)):
            event = 0 if step == 1 else 2 * (step - 1) - 1 + way
            name, ref, size, offset, sent = item
            base = blocks[event] * size + offset
            if step == half:
                cut = sent // 2
                part_ref = piece(ref, base + way * cut, None, cut, cut)
            else:
                part_ref = piece(ref, base, None, sent, sent)
            net.start((name, way, step), part_ref, part_ref, device)

    def ring_wait(item, step):
        for way, device in ((0, right), (1, left)):
            event = n - 1 if step == half else 2 * step - 1 + way
            net.arrived((item[0], way, step), ring_piece(item, event, way), device)

    def events_of(step):
        if step == 0:
            return [0]
        return [n - 1] if step == half else [2 * step - 1, 2 * step]

    def quarter(item, event, holder):
        name, ref, size, offset, sent = item
        return piece(ref, blocks[event] * size + holder * sent, None, sent, sent)

    split_items = [item for item, s in zip(factors, (splits[1], splits[0])) if s > 1]

    def share(step):
        for e in events_of(step) if step else []:
            for item in split_items:
                mine = quarter(item, e, tp)
                for d in range(1, pairs):
                    net.start((item[0], "x", d, e), mine, mine, {"tp": 2 * ((q + d) % pairs) + c})
                net.start((item[0], "c", 0, e), mine, mine, partner)

    def relay(step):
        for e in events_of(step) if step else []:
            for item in split_items:
                for d in range(1, pairs):
                    other = quarter(item, e, 2 * ((q + pairs - d) % pairs) + c)
                    net.arrived((item[0], "x", d, e), other, partner)
                    net.start((item[0], "c", d, e), other, other, partner)

    def gathered(step):
        for e in events_of(step) if step else []:
            for item in split_items:
                for d in range(pairs):
                    other = quarter(item, e, 2 * ((q + pairs - d) % pairs) + 1 - c)
                    net.arrived((item[0], "c", d, e), other, partner)

    tile = tile_of(tokens, 512)

    def project(step):
        for e in events_of(step):
            x_in[e].wait()
            at = span(blocks[e] * rows, rows, rows)

            def body(i, carry, e=e, at=at):
                r = span(i * tile, tile, tile)
                left_side = xbuf[e, r]
                for a in range(2):
                    got = jnp.dot(left_side, vg[a, at], preferred_element_type=F32)
                    if e == 0:
                        acc[a, r] = got
                    else:
                        acc[a, r] += got
                return carry

            lax.fori_loop(0, tokens // tile, body, 0)

    def project_point():
        xp_in.wait()

        def body(i, carry):
            r = span(i * tile, tile, tile)
            acc[2, r] = jnp.dot(xpbuf[r], pp[...], preferred_element_type=F32)
            return carry

        lax.fori_loop(0, tokens // tile, body, 0)

    outs = []

    def master_stage(step):
        for item in masters:
            ring_wait(item, step)
            if step < half:
                ring_send(item, step + 1)
        store_master(step)

    def store_master(step):
        for e in events_of(step):
            b, bp = span(blocks[e] * rows, rows, rows), span(blocks[e] * rows_p, rows_p, rows_p)
            outs.append(fetch(mvg.at[0, b], out_mv.at[b]))
            outs.append(fetch(mvg.at[1, b], out_mg.at[b]))
            outs.append(fetch(mpp.at[bp], out_mp.at[bp]))

    def master_first():
        for copy in master_in:
            copy.wait()
        mvg[0, own] = m32[0].astype(BF16)
        mvg[1, own] = m32[1].astype(BF16)
        mpp[own_p] = mp32[...].astype(BF16)

    for item in factors:
        ring_send(item, 1)
    share(0)
    master_first()
    project(0)
    for step in range(1, half + 1):
        for item in factors:
            ring_wait(item, step)
            if step < half:
                ring_send(item, step + 1)
        share(step)
        if step == half - 1:
            for item in masters:
                ring_send(item, 1)
            store_master(0)
        relay(step - 1)
        if step >= 3:
            gathered(step - 2)
            project(step - 2)
    relay(half)
    gathered(half - 1)
    project(half - 1)
    gathered(half)
    project(half)
    project_point()
    outs.append(fetch(vg.at[0], out_pv))
    outs.append(fetch(vg.at[1], out_pg))
    outs.append(fetch(pp, out_pp))

    for copy in y_in:
        copy.wait()
    lows[...] = jnp.zeros_like(lows)

    def contract(i, carry):
        r = span(i * tile, tile, tile)
        for a in range(3):
            value = acc[a, r]
            upper = value.astype(BF16)
            lower = (value - upper.astype(F32)).astype(BF16)
            cot = ybuf[a, r]
            dims = (((0,), (0,)), ((), ()))
            lows[a] += lax.dot_general(
                upper, cot, dims, preferred_element_type=F32
            ) + lax.dot_general(lower, cot, dims, preferred_element_type=F32)
        return carry

    lax.fori_loop(0, tokens // tile, contract, 0)
    for a in range(3):
        for b in range(n):
            low_send[b, a] = (lows[a, b * part : (b + 1) * part] / (tokens * n)).astype(BF16)
    for d in range(1, n):
        to = (fs + d) % n
        net.start(("low", d), low_send.at[to], low_recv.at[fs], {"fs": to})
    master_stage(1)
    mine = span(fs * part, part, part)
    for d in range(1, n):
        src = (fs + n - d) % n
        net.arrived(("low", d), low_recv.at[src], {"fs": src})
    for a, (first_old, second_old) in enumerate(((f0, s0), (f1, s1), (f2, s2))):
        low = lows[a, mine] / (tokens * n)
        for d in range(1, n):
            low = low + low_recv[(fs + d) % n, a].astype(F32)
        out_low[a] = low
        first = 0.8 * first_old[...] + 0.2 * low
        second = 0.9 * second_old[...] + 0.1 * low * low
        dir_all[fs, a] = (first / (jnp.sqrt(second) + 1e-08)).astype(BF16)
    for d in range(1, n):
        to = (fs + d) % n
        net.start(("dir", d), dir_all.at[fs], dir_all.at[fs], {"fs": to})
    if half >= 3:
        master_stage(2)
    for d in range(1, n):
        src = (fs + n - d) % n
        net.arrived(("dir", d), dir_all.at[src], {"fs": src})
    sums = []
    for a in range(3):
        whole = jnp.concatenate([dir_all[b, a].astype(F32) for b in range(n)], axis=0)
        out_dir[a] = whole.astype(BF16)
        size = rows if a < 2 else rows_p

        def square(i, total, a=a, size=size):
            r = span(i * size, size, size)
            block_ref = vg[a, r] if a < 2 else pp[r]
            full = jnp.dot(block_ref, out_dir[a], preferred_element_type=F32)
            return total + jnp.sum(full * full, axis=0, keepdims=True)

        total = lax.fori_loop(0, n, square, jnp.zeros((1, out_dir.shape[2]), F32))
        sums.append(jnp.sum(total, axis=1, keepdims=True))
    row = lax.broadcasted_iota(jnp.int32, ss_own.shape, 0)
    ss_own[...] = jnp.where(row == 0, sums[0], jnp.where(row == 1, sums[1], sums[2]))
    for d in range(1, m):
        net.start(("ss", d), ss_own, ss_all.at[tp], {"tp": (tp + d) % m})
    ss_all[tp] = ss_own[...]
    for d in range(1, m):
        src = (tp + m - d) % m
        net.arrived(("ss", d), ss_all.at[src], {"tp": src})
    total = ss_all[0]
    for t in range(1, m):
        total = total + ss_all[t]
    out_ss[...] = total
    for step in range(3 if half >= 3 else 2, half + 1):
        master_stage(step)
    net.drain()
    for copy in outs:
        copy.wait()


def finish(entries, *refs):
    whole, held, master, factor = refs[0:3], refs[3:6], refs[6:9], refs[9:12]
    low, direction, squares = refs[12:15]
    olds, outs = refs[15:21], refs[21:]
    for a in range(3):
        step = 0.1 * lax.rsqrt(squares[a : a + 1, 0:1] / entries[a] + 1e-06)
        own = jnp.dot(factor[a][...], direction[a], preferred_element_type=F32)
        outs[a][...] = master[a][...] - step * own
        full = jnp.dot(whole[a][...], direction[a], preferred_element_type=F32)
        outs[3 + a][...] = (held[a][...].astype(F32) - step * full).astype(BF16)

    @pl.when(pl.program_id(0) == 0)
    def _():
        for a in range(3):
            outs[6 + a][...] = 0.8 * olds[a][...] + 0.2 * low[a]
            outs[9 + a][...] = 0.9 * olds[3 + a][...] + 0.1 * low[a] * low[a]


def local(n, m, *args):
    x, yv, yg, xp, yp, mv, mg, mp, fv, fg, fp, f0, f1, f2, s0, s1, s2 = args
    tokens = x.shape[0]
    rows, rows_p, rank, width = fv.shape[0], fp.shape[0], fv.shape[1], yv.shape[1]
    depth, depth_p, part = rows * n, rows_p * n, rank // n
    splits = tuple(m if r % (32 * m) == 0 else 1 for r in (rows, rows_p))
    half = n // 2
    shared = sum(s > 1 for s in splits)
    remote = 4 * 2 * half + shared * (n - 1) * (2 * (m // 2) - 1) + 2 * (n - 1) + m - 1
    any_spec, vmem = pl.BlockSpec(memory_space=pl.ANY), pl.BlockSpec(memory_space=pltpu.VMEM)
    shape = jax.ShapeDtypeStruct
    pv, pg, pp, bv, bg, bp, low, direction, squares = pl.pallas_call(
        functools.partial(kernel, n, m, splits),
        out_shape=(
            shape((depth, rank), BF16), shape((depth, rank), BF16), shape((depth_p, rank), BF16),
            shape((depth, width), BF16), shape((depth, width), BF16), shape((depth_p, width), BF16),
            shape((3, part, width), F32), shape((3, rank, width), BF16), shape((8, 128), F32),
        ),
        in_specs=[any_spec] * 11 + [vmem] * 6,
        out_specs=(any_spec,) * 6 + (vmem,) * 3,
        scratch_shapes=[
            pltpu.VMEM((n, tokens, rows), BF16),
            pltpu.VMEM(xp.shape, BF16),
            pltpu.VMEM((3, tokens, width), BF16),
            pltpu.VMEM((2, depth, rank), BF16),
            pltpu.VMEM((depth_p, rank), BF16),
            pltpu.VMEM((2, depth, width), BF16),
            pltpu.VMEM((depth_p, width), BF16),
            pltpu.VMEM((2, rows, width), F32),
            pltpu.VMEM((rows_p, width), F32),
            pltpu.VMEM((3, tokens, rank), F32),
            pltpu.VMEM((3, rank, width), F32),
            pltpu.VMEM((n, 3, part, width), BF16),
            pltpu.VMEM((n, 3, part, width), BF16),
            pltpu.VMEM((n, 3, part, width), BF16),
            pltpu.VMEM((8, 128), F32),
            pltpu.VMEM((m, 8, 128), F32),
            pltpu.SemaphoreType.DMA((remote,)),
            pltpu.SemaphoreType.DMA((remote,)),
            pltpu.SemaphoreType.DMA((3 + 3 + n + 1 + 3 + 3 + 3 * n,)),
        ],
        compiler_params=pltpu.CompilerParams(
            collective_id=0, has_side_effects=True, vmem_limit_bytes=67043328
        ),
    )(x, xp, yv, yg, yp, mv, mg, mp, fv, fg, fp, f0, f1, f2, s0, s1, s2)

    steps = 4
    entries = (depth * width * m, depth * width * m, depth_p * width * m)

    def by_rows(array):
        return pl.BlockSpec((array.shape[0] // steps, array.shape[1]), lambda i: (i, 0))

    def fixed(array):
        return pl.BlockSpec(array.shape, lambda i: (0,) * len(array.shape))

    streamed = (pv, pg, pp, bv, bg, bp, mv, mg, mp, fv, fg, fp)
    kept = (low, direction, squares, f0, f1, f2, s0, s1, s2)
    results = tuple(shape(a.shape, F32) for a in (mv, mg, mp)) + tuple(
        shape(a.shape, BF16) for a in (bv, bg, bp)
    )
    small = tuple(shape(a.shape, F32) for a in (f0, f1, f2, s0, s1, s2))
    return pl.pallas_call(
        functools.partial(finish, entries),
        grid=(steps,),
        out_shape=results + small,
        in_specs=[by_rows(a) for a in streamed] + [fixed(a) for a in kept],
        out_specs=tuple(by_rows(a) for a in results) + tuple(fixed(a) for a in small),
        compiler_params=pltpu.CompilerParams(vmem_limit_bytes=50000000),
    )(*streamed, *kept)


def solution(mesh):
    rows, both, cols = P("fs", None), P("fs", "tp"), P(None, "tp")
    return jax.shard_map(
        functools.partial(local, mesh.shape["fs"], mesh.shape["tp"]),
        mesh=mesh,
        in_specs=(rows, both, both, rows, both, both, both, both, rows, rows, rows) + (both,) * 6,
        out_specs=(both,) * 3 + (cols,) * 3 + (both,) * 6,
        check_vma=False,
    )
```

```python
import functools

import jax
import jax.numpy as jnp
from jax import lax
from jax.experimental import pallas as pl
from jax.experimental.pallas import tpu as pltpu
from jax.sharding import PartitionSpec as P

MESH = pl.DeviceIdType.MESH
F32 = jnp.float32
BF16 = jnp.bfloat16


def tile_of(total, most):
    size = min(total, most)
    while total % size:
        size -= 8
    return size


def ring_position(index, n):
    half, odd = index // 2, index % 2
    return half + odd * (n - 1 - 2 * half)


def ring_index(position, n):
    back = position // (n // 2)
    return 2 * (position + back * (n - 1 - 2 * position)) + back


class Plan:
    def __init__(self, send, recv):
        self.send, self.recv, self.names, self.sent = send, recv, {}, []

    def copy(self, name, src, dst, device):
        slot = self.names.setdefault(name, len(self.names))
        return pltpu.make_async_remote_copy(
            src_ref=src, dst_ref=dst, send_sem=self.send.at[slot], recv_sem=self.recv.at[slot],
            device_id=device, device_id_type=MESH,
        )

    def start(self, name, src, dst, device):
        copy = self.copy(name, src, dst, device)
        copy.start()
        self.sent.append(copy)

    def arrived(self, name, dst, device):
        self.copy(name, dst, dst, device).wait_recv()

    def drain(self):
        for copy in self.sent:
            copy.wait_send()


def kernel(
    n, m, splits,
    x, xp, yv, yg, yp, mv, mg, mp, fv, fg, fp,
    f0, f1, f2, s0, s1, s2,
    out_pv, out_pg, out_pp, out_mv, out_mg, out_mp, out_low, out_dir, out_ss,
    xbuf, xpbuf, ybuf, vg, pp, mvg, mpp, m32, mp32, acc, lows, low_send, low_recv, dir_all, ss_own, ss_all,
    send, recv, local,
):
    fs, tp = lax.axis_index("fs"), lax.axis_index("tp")
    here = ring_position(fs, n)
    right = {"fs": ring_index((here + 1) % n, n)}
    left = {"fs": ring_index((here + n - 1) % n, n)}
    pairs = m // 2
    q, c = tp // 2, tp % 2
    partner = {"tp": 2 * q + 1 - c}
    rows, rows_p = fv.shape[0], fp.shape[0]
    tokens = x.shape[0]
    rank = vg.shape[2]
    part = rank // n
    half = n // 2
    net = Plan(send, recv)
    slots = iter(range(local.shape[0]))

    def fetch(src, dst):
        copy = pltpu.make_async_copy(src, dst, local.at[next(slots)])
        copy.start()
        return copy

    def block(event):
        if event == 0:
            return fs
        step = (event + 1) // 2
        return ring_index((here + (n - step if event % 2 else step)) % n, n)

    blocks = [block(e) for e in range(n)]

    def span(start, size, align):
        return pl.ds(pl.multiple_of(start, align), size)

    own = span(fs * rows, rows, rows)
    own_p = span(fs * rows_p, rows_p, rows_p)
    factor_in = [
        fetch(fp, pp.at[own_p]), fetch(fv, vg.at[0, own]), fetch(fg, vg.at[1, own]),
    ]
    master_in = [fetch(mv, m32.at[0]), fetch(mg, m32.at[1]), fetch(mp, mp32)]
    x_in = []
    for e in range(n):
        x_in.append(fetch(x.at[:, span(blocks[e] * rows, rows, rows)], xbuf.at[e]))
        if e == 0:
            xp_in = fetch(xp, xpbuf)
    y_in = [fetch(yv, ybuf.at[0]), fetch(yg, ybuf.at[1]), fetch(yp, ybuf.at[2])]

    barrier = pltpu.get_barrier_semaphore()
    for d in range(1, n):
        pl.semaphore_signal(barrier, inc=1, device_id={"fs": (fs + d) % n}, device_id_type=MESH)
    for d in range(1, m):
        pl.semaphore_signal(barrier, inc=1, device_id={"tp": (tp + d) % m}, device_id_type=MESH)
    for copy in factor_in:
        copy.wait()
    pl.semaphore_wait(barrier, n - 1 + m - 1)

    def piece(ref, owner, lo, size, align):
        if len(ref.shape) == 3:
            return ref.at[:, span(owner, size, align)] if lo is None else ref.at[:, span(owner + lo, size, align)]
        return ref.at[span(owner, size, align)] if lo is None else ref.at[span(owner + lo, size, align)]

    def stream(name, ref, size, split):
        sent = size // split
        offset = 0 if split == 1 else tp * sent
        return (name, ref, size, offset, sent)

    factors = [stream("p", pp, rows_p, splits[1]), stream("vg", vg, rows, splits[0])]
    masters = [stream("mvg", mvg, rows, 1), stream("mp", mpp, rows_p, 1)]

    def ring_piece(item, event, way):
        name, ref, size, offset, sent = item
        last = event == n - 1
        if last:
            cut = sent // 2
            return piece(ref, blocks[event] * size + offset + way * cut, None, cut, cut)
        return piece(ref, blocks[event] * size + offset, None, sent, sent)

    def ring_send(item, step):
        for way, device in ((0, right), (1, left)):
            event = 0 if step == 1 else 2 * (step - 1) - 1 + way
            name, ref, size, offset, sent = item
            base = blocks[event] * size + offset
            if step == half:
                cut = sent // 2
                part_ref = piece(ref, base + way * cut, None, cut, cut)
            else:
                part_ref = piece(ref, base, None, sent, sent)
            net.start((name, way, step), part_ref, part_ref, device)

    def ring_wait(item, step):
        for way, device in ((0, right), (1, left)):
            event = n - 1 if step == half else 2 * step - 1 + way
            net.arrived((item[0], way, step), ring_piece(item, event, way), device)

    def events_of(step):
        if step == 0:
            return [0]
        return [n - 1] if step == half else [2 * step - 1, 2 * step]

    def quarter(item, event, holder):
        name, ref, size, offset, sent = item
        return piece(ref, blocks[event] * size + holder * sent, None, sent, sent)

    split_items = [item for item, s in zip(factors, (splits[1], splits[0])) if s > 1]

    def share(step):
        for e in events_of(step) if step else []:
            for item in split_items:
                mine = quarter(item, e, tp)
                for d in range(1, pairs):
                    net.start((item[0], "x", d, e), mine, mine, {"tp": 2 * ((q + d) % pairs) + c})
                net.start((item[0], "c", 0, e), mine, mine, partner)

    def relay(step):
        for e in events_of(step) if step else []:
            for item in split_items:
                for d in range(1, pairs):
                    other = quarter(item, e, 2 * ((q + pairs - d) % pairs) + c)
                    net.arrived((item[0], "x", d, e), other, partner)
                    net.start((item[0], "c", d, e), other, other, partner)

    def gathered(step):
        for e in events_of(step) if step else []:
            for item in split_items:
                for d in range(pairs):
                    other = quarter(item, e, 2 * ((q + pairs - d) % pairs) + 1 - c)
                    net.arrived((item[0], "c", d, e), other, partner)

    tile = tile_of(tokens, 512)

    def project(step):
        for e in events_of(step):
            x_in[e].wait()
            at = span(blocks[e] * rows, rows, rows)

            def body(i, carry, e=e, at=at):
                r = span(i * tile, tile, tile)
                left_side = xbuf[e, r]
                for a in range(2):
                    got = jnp.dot(left_side, vg[a, at], preferred_element_type=F32)
                    if e == 0:
                        acc[a, r] = got
                    else:
                        acc[a, r] += got
                return carry

            lax.fori_loop(0, tokens // tile, body, 0)

    def project_point():
        xp_in.wait()

        def body(i, carry):
            r = span(i * tile, tile, tile)
            acc[2, r] = jnp.dot(xpbuf[r], pp[...], preferred_element_type=F32)
            return carry

        lax.fori_loop(0, tokens // tile, body, 0)

    outs = []

    def master_stage(step):
        for item in masters:
            ring_wait(item, step)
            if step < half:
                ring_send(item, step + 1)
        store_master(step)

    def store_master(step):
        for e in events_of(step):
            b, bp = span(blocks[e] * rows, rows, rows), span(blocks[e] * rows_p, rows_p, rows_p)
            outs.append(fetch(mvg.at[0, b], out_mv.at[b]))
            outs.append(fetch(mvg.at[1, b], out_mg.at[b]))
            outs.append(fetch(mpp.at[bp], out_mp.at[bp]))

    def master_first():
        for copy in master_in:
            copy.wait()
        mvg[0, own] = m32[0].astype(BF16)
        mvg[1, own] = m32[1].astype(BF16)
        mpp[own_p] = mp32[...].astype(BF16)

    for item in factors:
        ring_send(item, 1)
    share(0)
    master_first()
    project(0)
    for step in range(1, half + 1):
        for item in factors:
            ring_wait(item, step)
            if step < half:
                ring_send(item, step + 1)
        share(step)
        if step == half - 1:
            for item in masters:
                ring_send(item, 1)
            store_master(0)
        relay(step - 1)
        if step >= 3:
            gathered(step - 2)
            project(step - 2)
    relay(half)
    gathered(half - 1)
    project(half - 1)
    gathered(half)
    master_stage(1)
    project(half)
    project_point()
    outs.append(fetch(vg.at[0], out_pv))
    outs.append(fetch(vg.at[1], out_pg))
    outs.append(fetch(pp, out_pp))

    for copy in y_in:
        copy.wait()
    lows[...] = jnp.zeros_like(lows)

    def contract(i, carry):
        r = span(i * tile, tile, tile)
        for a in range(3):
            value = acc[a, r]
            upper = value.astype(BF16)
            lower = (value - upper.astype(F32)).astype(BF16)
            cot = ybuf[a, r]
            dims = (((0,), (0,)), ((), ()))
            lows[a] += lax.dot_general(
                upper, cot, dims, preferred_element_type=F32
            ) + lax.dot_general(lower, cot, dims, preferred_element_type=F32)
        return carry

    lax.fori_loop(0, tokens // tile, contract, 0)
    for a in range(3):
        for b in range(n):
            low_send[b, a] = (lows[a, b * part : (b + 1) * part] / (tokens * n)).astype(BF16)
    for d in range(1, n):
        to = (fs + d) % n
        net.start(("low", d), low_send.at[to], low_recv.at[fs], {"fs": to})
    mine = span(fs * part, part, part)
    for d in range(1, n):
        src = (fs + n - d) % n
        net.arrived(("low", d), low_recv.at[src], {"fs": src})
    for a, (first_old, second_old) in enumerate(((f0, s0), (f1, s1), (f2, s2))):
        low = lows[a, mine] / (tokens * n)
        for d in range(1, n):
            low = low + low_recv[(fs + d) % n, a].astype(F32)
        out_low[a] = low
        first = 0.8 * first_old[...] + 0.2 * low
        second = 0.9 * second_old[...] + 0.1 * low * low
        dir_all[fs, a] = (first / (jnp.sqrt(second) + 1e-08)).astype(BF16)
    for d in range(1, n):
        to = (fs + d) % n
        net.start(("dir", d), dir_all.at[fs], dir_all.at[fs], {"fs": to})
    if half >= 3:
        master_stage(2)
    for d in range(1, n):
        src = (fs + n - d) % n
        net.arrived(("dir", d), dir_all.at[src], {"fs": src})
    sums = []
    for a in range(3):
        whole = jnp.concatenate([dir_all[b, a].astype(F32) for b in range(n)], axis=0)
        out_dir[a] = whole.astype(BF16)
        size = rows if a < 2 else rows_p

        def square(i, total, a=a, size=size):
            r = span(i * size, size, size)
            block_ref = vg[a, r] if a < 2 else pp[r]
            full = jnp.dot(block_ref, out_dir[a], preferred_element_type=F32)
            return total + jnp.sum(full * full, axis=0, keepdims=True)

        total = lax.fori_loop(0, n, square, jnp.zeros((1, out_dir.shape[2]), F32))
        sums.append(jnp.sum(total, axis=1, keepdims=True))
    row = lax.broadcasted_iota(jnp.int32, ss_own.shape, 0)
    ss_own[...] = jnp.where(row == 0, sums[0], jnp.where(row == 1, sums[1], sums[2]))
    for d in range(1, m):
        net.start(("ss", d), ss_own, ss_all.at[tp], {"tp": (tp + d) % m})
    ss_all[tp] = ss_own[...]
    for d in range(1, m):
        src = (tp + m - d) % m
        net.arrived(("ss", d), ss_all.at[src], {"tp": src})
    total = ss_all[0]
    for t in range(1, m):
        total = total + ss_all[t]
    out_ss[...] = total
    for step in range(3 if half >= 3 else 2, half + 1):
        master_stage(step)
    net.drain()
    for copy in outs:
        copy.wait()


def finish(entries, *refs):
    whole, held, master, factor = refs[0:3], refs[3:6], refs[6:9], refs[9:12]
    low, direction, squares = refs[12:15]
    olds, outs = refs[15:21], refs[21:]
    for a in range(3):
        step = 0.1 * lax.rsqrt(squares[a : a + 1, 0:1] / entries[a] + 1e-06)
        own = jnp.dot(factor[a][...], direction[a], preferred_element_type=F32)
        outs[a][...] = master[a][...] - step * own
        full = jnp.dot(whole[a][...], direction[a], preferred_element_type=F32)
        outs[3 + a][...] = (held[a][...].astype(F32) - step * full).astype(BF16)

    @pl.when(pl.program_id(0) == 0)
    def _():
        for a in range(3):
            outs[6 + a][...] = 0.8 * olds[a][...] + 0.2 * low[a]
            outs[9 + a][...] = 0.9 * olds[3 + a][...] + 0.1 * low[a] * low[a]


def local(n, m, *args):
    x, yv, yg, xp, yp, mv, mg, mp, fv, fg, fp, f0, f1, f2, s0, s1, s2 = args
    tokens = x.shape[0]
    rows, rows_p, rank, width = fv.shape[0], fp.shape[0], fv.shape[1], yv.shape[1]
    depth, depth_p, part = rows * n, rows_p * n, rank // n
    splits = tuple(m if r % (32 * m) == 0 else 1 for r in (rows, rows_p))
    half = n // 2
    shared = sum(s > 1 for s in splits)
    remote = 4 * 2 * half + shared * (n - 1) * (2 * (m // 2) - 1) + 2 * (n - 1) + m - 1
    any_spec, vmem = pl.BlockSpec(memory_space=pl.ANY), pl.BlockSpec(memory_space=pltpu.VMEM)
    shape = jax.ShapeDtypeStruct
    pv, pg, pp, bv, bg, bp, low, direction, squares = pl.pallas_call(
        functools.partial(kernel, n, m, splits),
        out_shape=(
            shape((depth, rank), BF16), shape((depth, rank), BF16), shape((depth_p, rank), BF16),
            shape((depth, width), BF16), shape((depth, width), BF16), shape((depth_p, width), BF16),
            shape((3, part, width), F32), shape((3, rank, width), BF16), shape((8, 128), F32),
        ),
        in_specs=[any_spec] * 11 + [vmem] * 6,
        out_specs=(any_spec,) * 6 + (vmem,) * 3,
        scratch_shapes=[
            pltpu.VMEM((n, tokens, rows), BF16),
            pltpu.VMEM(xp.shape, BF16),
            pltpu.VMEM((3, tokens, width), BF16),
            pltpu.VMEM((2, depth, rank), BF16),
            pltpu.VMEM((depth_p, rank), BF16),
            pltpu.VMEM((2, depth, width), BF16),
            pltpu.VMEM((depth_p, width), BF16),
            pltpu.VMEM((2, rows, width), F32),
            pltpu.VMEM((rows_p, width), F32),
            pltpu.VMEM((3, tokens, rank), F32),
            pltpu.VMEM((3, rank, width), F32),
            pltpu.VMEM((n, 3, part, width), BF16),
            pltpu.VMEM((n, 3, part, width), BF16),
            pltpu.VMEM((n, 3, part, width), BF16),
            pltpu.VMEM((8, 128), F32),
            pltpu.VMEM((m, 8, 128), F32),
            pltpu.SemaphoreType.DMA((remote,)),
            pltpu.SemaphoreType.DMA((remote,)),
            pltpu.SemaphoreType.DMA((3 + 3 + n + 1 + 3 + 3 + 3 * n,)),
        ],
        compiler_params=pltpu.CompilerParams(
            collective_id=0, has_side_effects=True, vmem_limit_bytes=67043328
        ),
    )(x, xp, yv, yg, yp, mv, mg, mp, fv, fg, fp, f0, f1, f2, s0, s1, s2)

    steps = 4
    entries = (depth * width * m, depth * width * m, depth_p * width * m)

    def by_rows(array):
        return pl.BlockSpec((array.shape[0] // steps, array.shape[1]), lambda i: (i, 0))

    def fixed(array):
        return pl.BlockSpec(array.shape, lambda i: (0,) * len(array.shape))

    streamed = (pv, pg, pp, bv, bg, bp, mv, mg, mp, fv, fg, fp)
    kept = (low, direction, squares, f0, f1, f2, s0, s1, s2)
    results = tuple(shape(a.shape, F32) for a in (mv, mg, mp)) + tuple(
        shape(a.shape, BF16) for a in (bv, bg, bp)
    )
    small = tuple(shape(a.shape, F32) for a in (f0, f1, f2, s0, s1, s2))
    return pl.pallas_call(
        functools.partial(finish, entries),
        grid=(steps,),
        out_shape=results + small,
        in_specs=[by_rows(a) for a in streamed] + [fixed(a) for a in kept],
        out_specs=tuple(by_rows(a) for a in results) + tuple(fixed(a) for a in small),
        compiler_params=pltpu.CompilerParams(vmem_limit_bytes=67043328),
    )(*streamed, *kept)


def solution(mesh):
    rows, both, cols = P("fs", None), P("fs", "tp"), P(None, "tp")
    return jax.shard_map(
        functools.partial(local, mesh.shape["fs"], mesh.shape["tp"]),
        mesh=mesh,
        in_specs=(rows, both, both, rows, both, both, both, both, rows, rows, rows) + (both,) * 6,
        out_specs=(both,) * 3 + (cols,) * 3 + (both,) * 6,
        check_vma=False,
    )
```
